32 devices in a mesh: sp: 4 (over y, x), tp: 8 (over z, core).
Axes of the slice: x: 2, y: 2, z: 4, core: 2. Of those that a mesh axis runs over, the one named last changes fastest.
Arguments:
- tokens: bfloat16 [2048, 2048], P(('sp', 'tp')), may hold values from -6 to 6
- query_vectors: bfloat16 [2048, 2048], P('sp', 'tp'), may hold values from -8 to 8
- key_vectors: bfloat16 [2048, 2048], P('sp', 'tp'), may hold values from -8 to 8
- value_vectors: bfloat16 [2048, 2048], P('sp', 'tp'), may hold values from -24 to 24
- cum_gate: float32 [2048, 32], P('sp', 'tp'), may hold values from -260 to 0, as said below
- out_weight: bfloat16 [2048, 2048], P('tp'), may hold values from -0.125 to 0.125
- norm_gain: float32 [2048], replicated, may hold values from 0.1 to 1.9
- gate_weight: bfloat16 [4, 2048, 7168], P('sp', None, 'tp'), may hold values from -0.125 to 0.125
- up_weight: bfloat16 [4, 2048, 7168], P('sp', None, 'tp'), may hold values from -0.125 to 0.125
- down_weight: bfloat16 [4, 7168, 2048], P('sp', 'tp'), may hold values from -0.0625 to 0.0625
- expert_ids: int32 [2048, 2], P(('sp', 'tp')), may hold values from 0 to 3, all different within a row; in each aligned block of 64 rows (0 to 63, 64 to 127, ...) at most 48 rows name the same one
- route_weights: float32 [2048, 2], P(('sp', 'tp')), may hold values from 0.2 to 1
Outputs:
- layer_output: bfloat16 [2048, 2048], P(('sp', 'tp'))
The draws below stay inside these ranges and needn't reach their ends.
Inputs may be any that keep to these rules, and one draw needn't show every extreme that they name: `cum_gate`: along the positions each head's values never rise. `expert_ids`: within the rows of one device no expert is named by more than 48 rows, and in some devices' rows one expert is named by exactly 48; a row names 2 different experts.
All inputs are finite; a program needn't handle non-finite values.
Results may differ from the reference program's by a relative error of at most 0.014.
Values may be sent and summed in bfloat16 or wider, within the bound.
A program may use at most 128 MiB of HBM per device.

```python
import math
import jax
import jax.numpy as jnp
import numpy as np
from jax import lax

D = 2048
HEAD_COUNT = 32
HEAD_DIM = 64
FFE = 7168
TOP = 2
TOK_SP = 512
EXPERTS = 4
TOKEN_COUNT = 2048
TOK_DEV = 64
CAP = 48


def paired_draw(key):
    parallel_flows = jax.random.split(jax.random.fold_in(key, 101), 2)
    width = HEAD_COUNT * HEAD_DIM
    query_part = jax.random.truncated_normal(parallel_flows[0], -6.0, 6.0, (TOKEN_COUNT, width), jnp.float32)
    key_part = jax.random.truncated_normal(parallel_flows[1], -6.0, 6.0, (TOKEN_COUNT, width), jnp.float32)
    return (query_part, key_part)


def draw_query_vectors(key, part):
    query_part, key_part = paired_draw(key)
    return query_part.astype(jnp.bfloat16)


def draw_key_vectors(key, part):
    query_part, key_part = paired_draw(key)
    return key_part.astype(jnp.bfloat16)


def draw_cum_gate(key, part):
    parallel_flows = jax.random.split(jax.random.fold_in(key, 202), 7)
    slow_cut = 8
    slow = jax.random.randint(parallel_flows[0], (HEAD_COUNT,), 0, 16) < slow_cut
    fast_rate = jnp.exp(jax.random.uniform(parallel_flows[1], (HEAD_COUNT,), jnp.float32, math.log(1.0 / 100.0), math.log(1.0 / 30.0)))
    slow_rate = jnp.exp(jax.random.uniform(parallel_flows[2], (HEAD_COUNT,), jnp.float32, 0.0, math.log(3.0))) / TOKEN_COUNT
    rate = jnp.where(slow, slow_rate, fast_rate)
    blocks = TOKEN_COUNT // TOK_SP
    step_levels = 2.0 ** jnp.linspace(-1.0, 1.0, blocks)
    step_levels = step_levels[jax.random.permutation(parallel_flows[3], blocks)]
    factor = jnp.repeat(step_levels, TOK_SP)
    rough = jax.random.uniform(parallel_flows[4], (TOKEN_COUNT, HEAD_COUNT), jnp.float32, 0.3, 1.7)
    descending_steps = rate[None, :] * factor[:, None] * rough
    spike_position = jax.random.randint(parallel_flows[5], (4,), 0, TOKEN_COUNT)
    spike_penalty = -jnp.log(1.0 - jax.random.uniform(parallel_flows[6], (4, HEAD_COUNT), jnp.float32, 0.2, 0.5))
    descending_steps = descending_steps.at[spike_position].add(spike_penalty)
    return jnp.cumsum(-descending_steps, axis=0)


def level_of(rng, shape, cuts, least, top_value):
    gain, own = 1.0, jax.random.fold_in(rng, 6)
    for dim, parts in cuts:
        draws = jnp.exp(jax.random.uniform(jax.random.fold_in(own, dim), (parts,), jnp.float32, least / len(cuts), top_value / len(cuts)))
        gain = gain * jnp.repeat(draws, shape[dim] // parts).reshape([-1 if axis == dim else 1 for axis in range(len(shape))])
    return gain


def routed_block(key, own, number, rows, count, top, limit, slope):
    ranking = jax.random.permutation(key, count)
    crowded, ordinary = portions_of(count, rows * top, limit, slope, True), portions_of(count, rows * top, limit, slope, False)
    places = jnp.arange(count)

    def named(tallies, offset_by):
        used = int((tallies > 0).sum())
        fixed = max(1, used // 4)
        passed = fixed + (places - fixed + offset_by * (used - fixed)) % max(1, count - fixed)
        return jnp.zeros((count,), jnp.int32).at[ranking[jnp.where(places < fixed, places, passed)]].set(jnp.asarray(tallies, jnp.int32))

    tallies = jnp.where(number % 4 == 0, named(crowded, number // 4), named(ordinary, number - number // 4 - 1))
    mixed = jax.random.permutation(jax.random.fold_in(own, 3), count)
    giver, receiver = mixed[0:count // 2 * 2:2], mixed[1:count // 2 * 2:2]
    slack = jnp.minimum(tallies[giver] - 1, limit - tallies[receiver]) // 2
    slack = jnp.where((giver == ranking[0]) | (receiver == ranking[0]) | (tallies[receiver] == 0), 0, jnp.maximum(slack, 0))
    passed = jax.random.randint(jax.random.fold_in(own, 4), (count // 2,), 0, 1 << 20) % (slack + 1)
    tallies = tallies.at[giver].add(-passed).at[receiver].add(passed)
    items = jnp.searchsorted(jnp.cumsum(tallies), jnp.arange(rows * top), side="right").astype(jnp.int32)
    listing = items.reshape(top, rows).T
    listing = listing[jax.random.permutation(jax.random.fold_in(own, 1), rows)]
    offset_by = jax.random.randint(jax.random.fold_in(own, 2), (rows, 1), 0, top)
    return jnp.take_along_axis(listing, (jnp.arange(top)[None, :] + offset_by) % top, axis=1)


def portions_of(count, total, most, skew, full):
    weights = [(1 << 20) // math.isqrt(grade ** skew) + 1 for grade in range(1, count + 1)]
    largest = most if full else min(most, max(-(-total // count), total * weights[0] // sum(weights)))
    least = 1 if total - largest >= count - 1 else 0
    given, surplus = [largest] + [least] * (count - 1), total - largest - least * (count - 1)
    while surplus > 0:
        free = [i for i in range(1, count) if given[i] < largest] or [i for i in range(1, count) if given[i] < most]
        mass, left = sum([weights[i] for i in free]), surplus
        for i in free:
            addition = min(most - given[i], max(1, left * weights[i] // mass), surplus)
            given[i] = given[i] + addition
            surplus = surplus - addition
    return np.array(given)


def scatter_about(key, extent, spread, reach, cuts=(), kind=jnp.bfloat16):
    loudness = level_of(key, extent, cuts, -0.22, 0.18) if cuts else 1.0
    entries = jax.random.normal(key, extent, jnp.float32) * spread * loudness
    return jnp.minimum(jnp.maximum(entries, -reach), reach).astype(kind)


def setup_inputs(seed: int = 0) -> dict:
    key_list = jax.random.split(jax.random.key(seed), 13)
    tokens = scatter_about(key_list[0], (TOKEN_COUNT, D), 1.0, 6.0, ((0, 32),))
    query_vectors = draw_query_vectors(jax.random.fold_in(key_list[12], 71), 0)
    key_vectors = draw_key_vectors(jax.random.fold_in(key_list[12], 71), 0)
    value_vectors = scatter_about(key_list[3], (TOKEN_COUNT, HEAD_COUNT * HEAD_DIM), 4.0, 24.0, ((0, 4), (1, 8)))
    cum_gate = draw_cum_gate(jax.random.fold_in(key_list[12], 71), 0)
    out_weight = scatter_about(key_list[5], (HEAD_COUNT * HEAD_DIM, D), (HEAD_COUNT * HEAD_DIM) ** -0.5, 0.125, ((0, 8),))
    norm_gain = jnp.clip(1.0 + 0.18 * jax.random.normal(key_list[6], (D,), jnp.float32), 0.1, 1.9)
    gate_weight = scatter_about(key_list[7], (EXPERTS, D, FFE), D ** -0.5, 0.125, ((0, 4), (2, 8)))
    up_weight = scatter_about(key_list[8], (EXPERTS, D, FFE), D ** -0.5, 0.125, ((0, 4), (2, 8)))
    down_weight = scatter_about(key_list[9], (EXPERTS, FFE, D), FFE ** -0.5, 0.0625, ((0, 4), (1, 8)))
    expert_ids_keys = jax.random.split(jax.random.fold_in(key_list[10], 1), TOKEN_COUNT // TOK_DEV)
    expert_ids_turns = jax.random.permutation(jax.random.fold_in(key_list[10], 3), TOKEN_COUNT // TOK_DEV)
    expert_ids = jax.vmap(lambda own, number: routed_block(jax.random.fold_in(key_list[10], 2), own, number, TOK_DEV, EXPERTS, TOP, CAP, 1))(expert_ids_keys, expert_ids_turns).reshape((TOKEN_COUNT, TOP))
    route_weights = jnp.clip(0.2 + 0.8 * jax.random.uniform(key_list[11], (TOKEN_COUNT, TOP), jnp.float32) ** level_of(key_list[11], (TOKEN_COUNT, TOP), ((0, 32),), -0.2, 0.2), 0.2, 1.0)
    return {"tokens": tokens, "query_vectors": query_vectors, "key_vectors": key_vectors, "value_vectors": value_vectors, "cum_gate": cum_gate, "out_weight": out_weight, "norm_gain": norm_gain, "gate_weight": gate_weight, "up_weight": up_weight, "down_weight": down_weight, "expert_ids": expert_ids, "route_weights": route_weights}


def reference(tokens, query_vectors, key_vectors, value_vectors, cum_gate, out_weight, norm_gain, gate_weight, up_weight, down_weight, expert_ids, route_weights):
    score_scale = HEAD_DIM ** (-0.5)
    query_block = math.gcd(TOKEN_COUNT, 512)
    block_count = TOKEN_COUNT // query_block
    all_positions = jnp.arange(TOKEN_COUNT, dtype=jnp.int32)

    def head_output(head_index):
        column = (head_index * HEAD_DIM).astype(jnp.int32)
        query_head = lax.dynamic_slice_in_dim(query_vectors, column, HEAD_DIM, 1)
        key_head = lax.dynamic_slice_in_dim(key_vectors, column, HEAD_DIM, 1)
        value_head = lax.dynamic_slice_in_dim(value_vectors, column, HEAD_DIM, 1)
        gate_head = lax.dynamic_slice_in_dim(cum_gate, head_index.astype(jnp.int32), 1, 1)[:, 0]

        def block_output(block_index):
            first_row = (block_index * query_block).astype(jnp.int32)
            query_rows = lax.dynamic_slice_in_dim(query_head, first_row, query_block, 0)
            gate_rows = lax.dynamic_slice_in_dim(gate_head, first_row, query_block, 0)
            scores = jnp.dot(query_rows, key_head.T, preferred_element_type=jnp.float32) * score_scale
            scores = scores + gate_rows[:, None] - gate_head[None, :]
            query_pos = first_row + jnp.arange(query_block, dtype=jnp.int32)
            visible = all_positions[None, :] <= query_pos[:, None]
            scores = jnp.where(visible, scores, -jnp.inf)
            peak = lax.optimization_barrier(jnp.max(scores, axis=1, keepdims=True))
            exponent = jnp.exp(scores - peak)
            denominator = lax.optimization_barrier(jnp.sum(exponent, axis=1))
            probs = exponent.astype(jnp.bfloat16)
            summed = jnp.dot(probs, value_head, preferred_element_type=jnp.float32)
            return (summed / denominator[:, None]).astype(jnp.bfloat16)
        blocks = lax.map(block_output, jnp.arange(block_count, dtype=jnp.int32))
        return blocks.reshape(TOKEN_COUNT, HEAD_DIM)
    per_head = lax.map(head_output, jnp.arange(HEAD_COUNT, dtype=jnp.int32))
    attended = per_head.transpose(1, 0, 2).reshape(TOKEN_COUNT, HEAD_COUNT * HEAD_DIM)
    projected = jnp.dot(attended, out_weight, preferred_element_type=jnp.float32)
    stream = (tokens.astype(jnp.float32) + projected).astype(jnp.bfloat16)
    stream_wide = stream.astype(jnp.float32)
    inverse = lax.rsqrt(lax.optimization_barrier(jnp.mean(stream_wide * stream_wide, axis=1, keepdims=True)) + 1e-05)
    normed = (stream_wide * inverse * norm_gain[None, :]).astype(jnp.bfloat16)
    route_count = TOKEN_COUNT * TOP
    most_rows = TOKEN_COUNT // TOK_DEV * CAP
    flat_ids = expert_ids.reshape(-1)
    route_order = jnp.arange(route_count, dtype=jnp.int32)

    def expert_pass(routed_out, expert_index):
        sort_keys = jnp.where(flat_ids == expert_index, 0, 1) * route_count + route_order
        chosen = jnp.argsort(sort_keys)[:most_rows].astype(jnp.int32)
        valid = flat_ids[chosen] == expert_index
        rows_in = normed[chosen // TOP]
        gate_value = jnp.dot(rows_in, gate_weight[expert_index], preferred_element_type=jnp.float32)
        up_value = jnp.dot(rows_in, up_weight[expert_index], preferred_element_type=jnp.float32)
        hidden = (jax.nn.silu(gate_value) * up_value).astype(jnp.bfloat16)
        expert_out = jnp.dot(hidden, down_weight[expert_index], preferred_element_type=jnp.float32).astype(jnp.bfloat16)
        current = routed_out[chosen]
        routed_out = routed_out.at[chosen].set(jnp.where(valid[:, None], expert_out, current))
        return (routed_out, None)
    routed_out, _ = lax.scan(expert_pass, jnp.zeros((route_count, D), jnp.bfloat16), jnp.arange(EXPERTS, dtype=jnp.int32))
    routed = routed_out.reshape(TOKEN_COUNT, TOP, D).astype(jnp.float32)
    mixture = lax.optimization_barrier(jnp.sum(routed * route_weights[:, :, None], axis=1))
    return (stream_wide + mixture).astype(jnp.bfloat16)
```

```python
import functools
import math

import jax
import jax.numpy as jnp
from jax import lax
from jax.experimental import pallas as pl
from jax.experimental.pallas import tpu as pltpu
from jax.sharding import PartitionSpec as P

MESH = pl.DeviceIdType.MESH
VMEM_LIMIT = 60 * 1024 * 1024
F32 = jnp.float32
BF16 = jnp.bfloat16


def rcopy(src, dst, ssem, rsem, where):
    return pltpu.make_async_remote_copy(
        src_ref=src, dst_ref=dst, send_sem=ssem, recv_sem=rsem, device_id=where, device_id_type=MESH
    )


def vmem_specs(count):
    return [pl.BlockSpec(memory_space=pltpu.VMEM)] * count


def exchange_kernel(sp, k, v, g, ka, va, ga, ssem, rsem):
    s = lax.axis_index("sp")
    barrier = pltpu.get_barrier_semaphore()
    for d in range(1, sp):
        pl.semaphore_signal(barrier, inc=1, device_id={"sp": lax.rem(s + d, sp)}, device_id_type=MESH)
    pl.semaphore_wait(barrier, sp - 1)
    pairs = ((k, ka), (v, va), (g, ga))

    def copy(n, d, slot, target):
        src, dst = pairs[n]
        return rcopy(src, dst.at[slot], ssem.at[n, d], rsem.at[n, d], {"sp": target})

    for d in range(1, sp):

        @pl.when(s + d < sp)
        def _():
            for n in range(3):
                copy(n, d, s, s + d).start()

    for src, dst in pairs:
        dst[s] = src[...]
    for d in range(1, sp):

        @pl.when(s - d >= 0)
        def _():
            for n in range(3):
                copy(n, d, s - d, lax.rem(s + d, sp)).wait_recv()

    for d in range(1, sp):

        @pl.when(s + d < sp)
        def _():
            for n in range(3):
                copy(n, d, s, s + d).wait_send()


def attend_kernel(heads, q, ka, va, ga, w, out, att):
    s = lax.axis_index("sp")
    rows, width = q.shape
    hd = width // heads
    tile = math.gcd(rows, 256)
    log2e = 1.4426950408889634
    coef = hd ** (-0.5) * log2e
    for h in range(heads):
        cols = slice(h * hd, (h + 1) * hd)
        for i in range(rows // tile):
            qt = q[i * tile : (i + 1) * tile, cols]
            seen = (i + 1) * tile

            def scores(kb, gb):
                return (
                    lax.dot_general(qt, kb, (((1,), (1,)), ((), ())), preferred_element_type=F32) * coef
                    - gb * log2e
                )

            sc = scores(ka[s, 0:seen, cols], ga[s, h : h + 1, 0:seen])
            row = lax.broadcasted_iota(jnp.int32, sc.shape, 0) + i * tile
            col = lax.broadcasted_iota(jnp.int32, sc.shape, 1)
            sc = jnp.where(col <= row, sc, -1e30)
            peak = jnp.max(sc, axis=1, keepdims=True)
            ex = jnp.exp2(sc - peak)
            total = jnp.sum(ex, axis=1, keepdims=True)
            acc = jnp.dot(ex.astype(BF16), va[s, 0:seen, cols], preferred_element_type=F32)

            def step(b, carry):
                peak, total, acc = carry
                sc = scores(ka[b, :, cols], ga[b, h : h + 1, :])
                new = jnp.maximum(peak, jnp.max(sc, axis=1, keepdims=True))
                ex = jnp.exp2(sc - new)
                fix = jnp.exp2(peak - new)
                total = total * fix + jnp.sum(ex, axis=1, keepdims=True)
                acc = acc * fix + jnp.dot(ex.astype(BF16), va[b, :, cols], preferred_element_type=F32)
                return new, total, acc

            peak, total, acc = lax.fori_loop(0, s, step, (peak, total, acc))
            att[i * tile : (i + 1) * tile, cols] = (acc / total).astype(BF16)
    wide = w.shape[1]
    chunk = math.gcd(wide, 512)
    for n in range(wide // chunk):
        cut = slice(n * chunk, (n + 1) * chunk)
        out[:, cut] = jnp.dot(att[...], w[:, cut], preferred_element_type=F32).astype(BF16)


def greet(sp, zn, s, z, c, partner):
    barrier = pltpu.get_barrier_semaphore()
    pl.semaphore_signal(barrier, inc=1, device_id={"tp": partner}, device_id_type=MESH)
    for i in range(1, zn):
        pl.semaphore_signal(
            barrier, inc=1, device_id={"tp": 2 * lax.rem(z + i, zn) + c}, device_id_type=MESH
        )
    for d in range(1, sp):
        pl.semaphore_signal(barrier, inc=1, device_id={"sp": lax.rem(s + d, sp)}, device_id_type=MESH)
    pl.semaphore_wait(barrier, 1 + (zn - 1) + (sp - 1))


def dispatch_kernel(
    sp, zn, p, tok, gain, place, comb, stream, rows, combs,
    xr, cb, zr, ng, pg, db, xs, xrs, as_, ars, zs, zrs, ns, nrs, ds_, drs, fs, frs,
):
    s, t = lax.axis_index("sp"), lax.axis_index("tp")
    z, c = t // 2, lax.rem(t, 2)
    partner = t + 1 - 2 * c
    T = tok.shape[0]
    cap = rows.shape[3]
    greet(sp, zn, s, z, c, partner)

    def at_z(i):
        return 2 * lax.rem(z + i, zn) + c

    def swap(i):
        zz = lax.rem(z + 1 + i, zn)
        src = p.at[pl.ds(pl.multiple_of((2 * zz + 1 - c) * T, 16), T)]
        return rcopy(src, xr.at[i], xs.at[i], xrs.at[i], {"tp": partner})

    def aux(n, i):
        src, dst = ((place, pg), (comb, combs))[n]
        return rcopy(src, dst.at[i], as_.at[n, i], ars.at[n, i], {"tp": at_z(i)})

    def reduce_to(i):
        return rcopy(cb.at[i], zr.at[i], zs.at[i], zrs.at[i], {"tp": at_z(1 + i)})

    def spread(i):
        return rcopy(ng.at[0], ng.at[i], ns.at[i], nrs.at[i], {"tp": at_z(i)})

    def route(i, d):
        e = lax.rem(s + d, sp)
        return rcopy(db.at[i, e], rows.at[s, c, i], ds_.at[i, d], drs.at[i, d], {"sp": e})

    def routed_slot(i, d):
        return rows.at[lax.rem(s + sp - d, sp), c, i]

    def forward(i, d):
        ref = routed_slot(i, d)
        return rcopy(ref, ref, fs.at[i, d], frs.at[i, d], {"tp": partner})

    for i in range(zn):
        swap(i).start()
    for i in range(1, zn):
        for n in range(2):
            aux(n, i).start()
    pg[0] = place[...]
    combs[0] = comb[...]
    own = None
    for i in range(zn):
        swap(i).wait_recv()
        zz = lax.rem(z + 1 + i, zn)
        both = p[pl.ds(pl.multiple_of((2 * zz + c) * T, 16), T), :].astype(F32) + xr[i].astype(F32)
        if i < zn - 1:
            cb[i] = both.astype(BF16)
            reduce_to(i).start()
        else:
            own = both
    for i in range(zn - 1):
        reduce_to(i).wait_recv()
        own = own + zr[i].astype(F32)
    st = (tok[...].astype(F32) + own).astype(BF16)
    stream[...] = st
    wide = st.astype(F32)
    inverse = lax.rsqrt(jnp.mean(wide * wide, axis=1, keepdims=True) + 1e-05)
    ng[0] = (wide * inverse * gain[...]).astype(BF16)
    for i in range(1, zn):
        spread(i).start()
    for i in range(zn):
        if i > 0:
            aux(0, i).wait_recv()
            spread(i).wait_recv()
        moved = jnp.dot(pg[i], ng[i], preferred_element_type=F32).astype(BF16)
        for e in range(sp):
            db[i, e] = moved[e * cap : (e + 1) * cap]
        for d in range(1, sp):
            route(i, d).start()
        rows[s, c, i] = db[i, s]
        forward(i, 0).start()
    for i in range(zn):

        def arrive(d, _):
            rcopy(
                db.at[i, 0], routed_slot(i, d), ds_.at[i, d], drs.at[i, d], {"sp": lax.rem(s + d, sp)}
            ).wait_recv()
            forward(i, d).start()
            return 0

        lax.fori_loop(1, sp, arrive, 0)
    for i in range(zn):

        def landed(d, _):
            ref = rows.at[lax.rem(s + sp - d, sp), 1 - c, i]
            rcopy(ref, ref, fs.at[i, d], frs.at[i, d], {"tp": partner}).wait_recv()
            forward(i, d).wait_send()
            return 0

        lax.fori_loop(0, sp, landed, 0)
        swap(i).wait_send()
        if i < zn - 1:
            reduce_to(i).wait_send()
        if i > 0:
            spread(i).wait_send()
            aux(1, i).wait_recv()
            for n in range(2):
                aux(n, i).wait_send()
        for d in range(1, sp):
            route(i, d).wait_send()


def combine_kernel(
    sp, zn, y, combs, stream, out, pr, cs, eb, mb, rr, ps, prs, es, ers, ms, mrs
):
    s, t = lax.axis_index("sp"), lax.axis_index("tp")
    z, c = t // 2, lax.rem(t, 2)
    partner = t + 1 - 2 * c
    T = stream.shape[0]
    cap, wide = y.shape[3], y.shape[4]
    greet(sp, zn, s, z, c, partner)
    order = list(range(1, zn)) + [0]

    def peer(d):
        return lax.rem(s + d, sp)

    def swap(i, d):
        return rcopy(y.at[peer(d), 1 - c, i], pr.at[i, d], ps.at[i, d], prs.at[i, d], {"tp": partner})

    def back(i, d, slot):
        return rcopy(cs.at[i, d], eb.at[i, slot], es.at[i, d], ers.at[i, d], {"sp": peer(d)})

    def reduce_to(i):
        return rcopy(
            mb.at[i], rr.at[i], ms.at[i], mrs.at[i], {"tp": 2 * lax.rem(z + zn - i, zn) + c}
        )

    for i in order:
        for d in list(range(1, sp)) + [0]:
            swap(i, d).start()
    for i in order:

        def both(d):
            swap(i, d).wait_recv()
            return (y[peer(d), c, i].astype(F32) + pr[i, d].astype(F32)).astype(BF16)

        def send(d, _):
            cs[i, d] = both(d)
            back(i, d, s).start()
            return 0

        lax.fori_loop(1, sp, send, 0)
        eb[i, s] = both(0)
    own = None
    for i in order:
        for d in range(1, sp):
            back(i, d, lax.rem(s + sp - d, sp)).wait_recv()
        parts = eb[i].reshape(sp * cap, wide)
        mixed = jnp.dot(combs[i], parts, preferred_element_type=F32)
        mixed = mixed[0:T] + mixed[T : 2 * T]
        if i > 0:
            mb[i] = mixed.astype(BF16)
            reduce_to(i).start()
        else:
            own = mixed
    for i in range(1, zn):
        reduce_to(i).wait_recv()
        own = own + rr[i].astype(F32)
    out[...] = (stream[...].astype(F32) + own).astype(BF16)
    for i in range(zn):
        for d in range(sp):
            swap(i, d).wait_send()
            if d > 0:
                back(i, d, s).wait_send()
        if i > 0:
            reduce_to(i).wait_send()


def params(cid=None):
    if cid is None:
        return pltpu.CompilerParams(vmem_limit_bytes=VMEM_LIMIT)
    return pltpu.CompilerParams(
        collective_id=cid, has_side_effects=True, vmem_limit_bytes=VMEM_LIMIT
    )


def shards(
    tokens,
    query_vectors,
    key_vectors,
    value_vectors,
    cum_gate,
    out_weight,
    norm_gain,
    gate_weight,
    up_weight,
    down_weight,
    expert_ids,
    route_weights,
):
    sp = lax.axis_size("sp")
    tp = lax.axis_size("tp")
    zn = tp // 2
    seg, width = query_vectors.shape
    heads = cum_gate.shape[1]
    T, D = tokens.shape
    dma = pltpu.SemaphoreType.DMA

    n_experts = gate_weight.shape[0] * sp
    top = expert_ids.shape[1]
    cap = max(2, 3 * T * top // (2 * n_experts))
    cap = -(-cap // 16) * 16
    slots = n_experts * cap
    flat = expert_ids.reshape(-1)
    hits = (flat[:, None] == jnp.arange(n_experts, dtype=jnp.int32)[None, :]).astype(F32)
    lower = jnp.tril(jnp.ones((flat.shape[0], flat.shape[0]), F32), -1)
    earlier = jnp.dot(lower, hits, preferred_element_type=F32)
    slot = (flat * cap + jnp.sum(earlier * hits, axis=1).astype(jnp.int32)).reshape(T, top)
    match = slot[:, :, None] == jnp.arange(slots, dtype=jnp.int32)[None, None, :]
    place = jnp.any(match, axis=1).astype(BF16).T
    weight = jnp.sum(jnp.where(match, route_weights[:, :, None], 0.0), axis=1)
    high = lax.reduce_precision(weight, 8, 7)
    comb = jnp.concatenate([high, weight - high], axis=0).astype(BF16)

    kall, vall, gall = pl.pallas_call(
        functools.partial(exchange_kernel, sp),
        out_shape=(
            jax.ShapeDtypeStruct((sp, seg, width), BF16),
            jax.ShapeDtypeStruct((sp, seg, width), BF16),
            jax.ShapeDtypeStruct((sp, heads, seg), F32),
        ),
        in_specs=vmem_specs(3),
        out_specs=tuple(vmem_specs(3)),
        scratch_shapes=[dma((3, sp)), dma((3, sp))],
        compiler_params=params(0),
        name="exchange",
    )(key_vectors, value_vectors, cum_gate.T)

    partial = pl.pallas_call(
        functools.partial(attend_kernel, heads),
        out_shape=jax.ShapeDtypeStruct((seg, D), BF16),
        in_specs=vmem_specs(5),
        out_specs=vmem_specs(1)[0],
        scratch_shapes=[pltpu.VMEM((seg, width), BF16)],
        compiler_params=params(),
        name="attend",
    )(query_vectors, kall, vall, gall, out_weight)

    stream, rows, combs = pl.pallas_call(
        functools.partial(dispatch_kernel, sp, zn),
        out_shape=(
            jax.ShapeDtypeStruct((T, D), BF16),
            jax.ShapeDtypeStruct((sp, 2, zn, cap, D), BF16),
            jax.ShapeDtypeStruct((zn, 2 * T, slots), BF16),
        ),
        in_specs=vmem_specs(5),
        out_specs=tuple(vmem_specs(3)),
        scratch_shapes=[
            pltpu.VMEM((zn, T, D), BF16),
            pltpu.VMEM((zn, T, D), BF16),
            pltpu.VMEM((zn, T, D), BF16),
            pltpu.VMEM((zn, T, D), BF16),
            pltpu.VMEM((zn, slots, T), BF16),
            pltpu.VMEM((zn, sp, cap, D), BF16),
            dma((zn,)), dma((zn,)),
            dma((2, zn)), dma((2, zn)),
            dma((zn,)), dma((zn,)),
            dma((zn,)), dma((zn,)),
            dma((zn, sp)), dma((zn, sp)),
            dma((zn, sp)), dma((zn, sp)),
        ],
        compiler_params=params(1),
        name="dispatch",
    )(partial, tokens, norm_gain[None, :], place, comb)

    flat_rows = rows.reshape(-1, D)
    gate_value = jnp.dot(flat_rows, gate_weight[0], preferred_element_type=F32)
    up_value = jnp.dot(flat_rows, up_weight[0], preferred_element_type=F32)
    hidden = (jax.nn.silu(gate_value) * up_value).astype(BF16)
    y = jnp.dot(hidden, down_weight[0], preferred_element_type=F32).astype(BF16)

    return pl.pallas_call(
        functools.partial(combine_kernel, sp, zn),
        out_shape=jax.ShapeDtypeStruct((T, D), BF16),
        in_specs=vmem_specs(3),
        out_specs=vmem_specs(1)[0],
        scratch_shapes=[
            pltpu.VMEM((zn, sp, cap, D), BF16),
            pltpu.VMEM((zn, sp, cap, D), BF16),
            pltpu.VMEM((zn, sp, cap, D), BF16),
            pltpu.VMEM((zn, T, D), BF16),
            pltpu.VMEM((zn, T, D), BF16),
            dma((zn, sp)), dma((zn, sp)),
            dma((zn, sp)), dma((zn, sp)),
            dma((zn,)), dma((zn,)),
        ],
        compiler_params=params(2),
        name="combine",
    )(y.reshape(rows.shape), combs, stream)


def solution(mesh):
    in_specs = (
        P(("sp", "tp"), None),
        P("sp", "tp"),
        P("sp", "tp"),
        P("sp", "tp"),
        P("sp", "tp"),
        P("tp", None),
        P(),
        P("sp", None, "tp"),
        P("sp", None, "tp"),
        P("sp", "tp", None),
        P(("sp", "tp"), None),
        P(("sp", "tp"), None),
    )
    out_specs = P(("sp", "tp"), None)
    return jax.shard_map(shards, mesh=mesh, in_specs=in_specs, out_specs=out_specs, check_vma=False)
```

```python
import functools
import math

import jax
import jax.numpy as jnp
from jax import lax
from jax.experimental import pallas as pl
from jax.experimental.pallas import tpu as pltpu
from jax.sharding import PartitionSpec as P

MESH = pl.DeviceIdType.MESH
VMEM_LIMIT = 60 * 1024 * 1024
F32 = jnp.float32
BF16 = jnp.bfloat16


def rcopy(src, dst, ssem, rsem, where):
    return pltpu.make_async_remote_copy(
        src_ref=src, dst_ref=dst, send_sem=ssem, recv_sem=rsem, device_id=where, device_id_type=MESH
    )


def vmem_specs(count):
    return [pl.BlockSpec(memory_space=pltpu.VMEM)] * count


def attend_kernel(sp, heads, q, k, v, g, w, out, ka, va, ga, att, top_s, sum_s, acc_s, ssem, rsem):
    s = lax.axis_index("sp")
    barrier = pltpu.get_barrier_semaphore()
    for d in range(1, sp):
        pl.semaphore_signal(barrier, inc=1, device_id={"sp": lax.rem(s + d, sp)}, device_id_type=MESH)
    pl.semaphore_wait(barrier, sp - 1)
    pairs = ((k, ka), (v, va), (g, ga))

    def copy(n, d):
        src, dst = pairs[n]
        return rcopy(src, dst.at[d], ssem.at[n, d], rsem.at[n, d], {"sp": lax.rem(s + d, sp)})

    for d in range(1, sp):

        @pl.when(s + d < sp)
        def _():
            for n in range(3):
                copy(n, d).start()

    rows, width = q.shape
    hd = width // heads
    tile = math.gcd(rows, 256)
    log2e = 1.4426950408889634
    coef = hd ** (-0.5) * log2e
    units = [(h, i) for h in range(heads) for i in range(rows // tile)]

    def scores(h, i, kb, gb):
        qt = q[i * tile : (i + 1) * tile, h * hd : (h + 1) * hd]
        return (
            lax.dot_general(qt, kb, (((1,), (1,)), ((), ())), preferred_element_type=F32) * coef
            - gb * log2e
        )

    for h, i in units:
        cols = slice(h * hd, (h + 1) * hd)
        seen = (i + 1) * tile
        sc = scores(h, i, k[0:seen, cols], g[h : h + 1, 0:seen])
        row = lax.broadcasted_iota(jnp.int32, sc.shape, 0) + i * tile
        col = lax.broadcasted_iota(jnp.int32, sc.shape, 1)
        sc = jnp.where(col <= row, sc, -1e30)
        peak = jnp.max(sc, axis=1, keepdims=True)
        ex = jnp.exp2(sc - peak)
        at = slice(i * tile, seen)
        top_s[h, at] = peak
        sum_s[h, at] = jnp.sum(ex, axis=1, keepdims=True)
        acc_s[h, at] = jnp.dot(ex.astype(BF16), v[0:seen, cols], preferred_element_type=F32)

    def step(d, _):
        for n in range(3):
            copy(n, d).wait_recv()
        for h, i in units:
            cols = slice(h * hd, (h + 1) * hd)
            at = slice(i * tile, (i + 1) * tile)
            sc = scores(h, i, ka[d, :, cols], ga[d, h : h + 1, :])
            peak = top_s[h, at]
            new = jnp.maximum(peak, jnp.max(sc, axis=1, keepdims=True))
            ex = jnp.exp2(sc - new)
            fix = jnp.exp2(peak - new)
            top_s[h, at] = new
            sum_s[h, at] = sum_s[h, at] * fix + jnp.sum(ex, axis=1, keepdims=True)
            acc_s[h, at] = acc_s[h, at] * fix + jnp.dot(
                ex.astype(BF16), va[d, :, cols], preferred_element_type=F32
            )
        return 0

    lax.fori_loop(1, s + 1, step, 0)
    for h, i in units:
        at = slice(i * tile, (i + 1) * tile)
        att[at, h * hd : (h + 1) * hd] = (acc_s[h, at] / sum_s[h, at]).astype(BF16)
    wide = w.shape[1]
    chunk = math.gcd(wide, 512)
    for n in range(wide // chunk):
        cut = slice(n * chunk, (n + 1) * chunk)
        out[:, cut] = jnp.dot(att[...], w[:, cut], preferred_element_type=F32).astype(BF16)
    for d in range(1, sp):

        @pl.when(s + d < sp)
        def _():
            for n in range(3):
                copy(n, d).wait_send()


def greet(sp, zn, s, z, c, partner):
    barrier = pltpu.get_barrier_semaphore()
    pl.semaphore_signal(barrier, inc=1, device_id={"tp": partner}, device_id_type=MESH)
    for i in range(1, zn):
        pl.semaphore_signal(
            barrier, inc=1, device_id={"tp": 2 * lax.rem(z + i, zn) + c}, device_id_type=MESH
        )
    for d in range(1, sp):
        pl.semaphore_signal(barrier, inc=1, device_id={"sp": lax.rem(s + d, sp)}, device_id_type=MESH)
    pl.semaphore_wait(barrier, 1 + (zn - 1) + (sp - 1))


def experts_kernel(
    sp, zn, p, tok, gain, place, comb, wg_in, wu_in, wd_in, out,
    wg, wu, wd, xr, cb, zr, ng, pg, combs, db, rows, hid, y, pr, cs, eb, mb, rr, keep,
    ws, xs, xrs, as_, ars, zs, zrs, ns, nrs, ds_, drs, fs, frs, ps, prs, es, ers, ms, mrs,
):
    s, t = lax.axis_index("sp"), lax.axis_index("tp")
    z, c = t // 2, lax.rem(t, 2)
    partner = t + 1 - 2 * c
    T, D = tok.shape
    cap = rows.shape[3]
    loads = [
        pltpu.make_async_copy(a.at[0], b, ws.at[n])
        for n, (a, b) in enumerate(((wg_in, wg), (wu_in, wu), (wd_in, wd)))
    ]
    for load in loads:
        load.start()
    greet(sp, zn, s, z, c, partner)
    offs = [0] + sorted(range(1, zn), key=lambda i: -min(i, zn - i))
    outs = offs[1:] + [0]

    def at_z(i):
        return 2 * lax.rem(z + i, zn) + c

    def peer(d):
        return lax.rem(s + d, sp)

    def behind(d):
        return lax.rem(s + sp - d, sp)

    def swap(i):
        zz = lax.rem(z + outs[i], zn)
        src = p.at[pl.ds(pl.multiple_of((2 * zz + 1 - c) * T, 16), T)]
        return rcopy(src, xr.at[i], xs.at[i], xrs.at[i], {"tp": partner})

    def aux(n, i):
        src, dst = ((place, pg), (comb, combs))[n]
        return rcopy(src, dst.at[i], as_.at[n, i], ars.at[n, i], {"tp": at_z(offs[i])})

    def reduce_to(i):
        return rcopy(cb.at[i], zr.at[i], zs.at[i], zrs.at[i], {"tp": at_z(outs[i])})

    def spread(i):
        return rcopy(ng.at[0], ng.at[i], ns.at[i], nrs.at[i], {"tp": at_z(offs[i])})

    def route(i, d):
        return rcopy(
            db.at[i, peer(d)], rows.at[i, s, c], ds_.at[i, d], drs.at[i, d], {"sp": peer(d)}
        )

    def routed(i, d):
        return rcopy(
            db.at[i, peer(d)], rows.at[i, behind(d), c], ds_.at[i, d], drs.at[i, d], {"sp": peer(d)}
        )

    def forward(i, d):
        ref = rows.at[i, behind(d), c]
        return rcopy(ref, ref, fs.at[i, d], frs.at[i, d], {"tp": partner})

    def forwarded(i, d):
        ref = rows.at[i, behind(d), 1 - c]
        return rcopy(ref, ref, fs.at[i, d], frs.at[i, d], {"tp": partner})

    def swap_out(i, d):
        return rcopy(y.at[i, peer(d), 1 - c], pr.at[i, d], ps.at[i, d], prs.at[i, d], {"tp": partner})

    def back(i, d, slot):
        return rcopy(cs.at[i, d], eb.at[i, slot], es.at[i, d], ers.at[i, d], {"sp": peer(d)})

    def reduce_out(i):
        return rcopy(
            mb.at[i], rr.at[i], ms.at[i], mrs.at[i], {"tp": at_z(zn - offs[i])}
        )

    def dispatch(i):
        if i > 0:
            aux(0, i).wait_recv()
            spread(i).wait_recv()
        moved = jnp.dot(pg[i], ng[i], preferred_element_type=F32)
        for e in range(sp):
            db[i, e] = moved[e * cap : (e + 1) * cap].astype(BF16)
        for d in range(1, sp):
            route(i, d).start()
        rows[i, s, c] = db[i, s]
        forward(i, 0).start()

    def pass_on(i):
        def arrive(d, _):
            routed(i, d).wait_recv()
            forward(i, d).start()
            return 0

        lax.fori_loop(1, sp, arrive, 0)

    def each(count, body):
        if count * rows.shape[1] <= 64:
            for n in range(count):
                body(n)
        else:
            lax.fori_loop(0, count, lambda n, _: (body(n), 0)[1], 0)

    def expert(i):
        def landed(d, _):
            forwarded(i, d).wait_recv()
            return 0

        lax.fori_loop(0, sp, landed, 0)
        x = rows.at[i]
        many = sp * 2 * cap
        units = wg.shape[1]
        step = 256

        def into(start, size):
            cut = pl.ds(start, size)
            xv = x[...].reshape(many, D)
            gate = jnp.dot(xv, wg[:, cut], preferred_element_type=F32)
            up = jnp.dot(xv, wu[:, cut], preferred_element_type=F32)
            hid[:, cut] = (gate / (1.0 + jnp.exp(-gate)) * up).astype(BF16)

        each(units // step, lambda n: into(pl.multiple_of(n * step, step), step))
        if units % step:
            into(units - units % step, units % step)
        chunk = math.gcd(D, 512)

        def down(n):
            cut = pl.ds(pl.multiple_of(n * chunk, chunk), chunk)
            got = jnp.dot(hid[...], wd[:, cut], preferred_element_type=F32).astype(BF16)
            y[i, :, :, :, cut] = got.reshape(sp, 2, cap, chunk)

        each(D // chunk, down)
        for d in list(range(1, sp)) + [0]:
            swap_out(i, d).start()

    def give_back(i):
        def both(d):
            swap_out(i, d).wait_recv()
            return (y[i, peer(d), c].astype(F32) + pr[i, d].astype(F32)).astype(BF16)

        def send(d, _):
            cs[i, d] = both(d)
            back(i, d, s).start()
            return 0

        lax.fori_loop(1, sp, send, 0)
        eb[i, s] = both(0)

    def mix(i):
        if i > 0:
            aux(1, i).wait_recv()
        for d in range(1, sp):
            back(i, d, behind(d)).wait_recv()
        mixed = jnp.dot(combs[i], eb[i].reshape(sp * cap, D), preferred_element_type=F32)
        mixed = mixed[0:T] + mixed[T : 2 * T]
        if i > 0:
            mb[i] = mixed.astype(BF16)
            reduce_out(i).start()
        else:
            keep[...] = mixed

    for i in range(zn):
        swap(i).start()
    for i in range(1, zn):
        for n in range(2):
            aux(n, i).start()
    pg[0] = place[...]
    combs[0] = comb[...]
    own = None
    for i in range(zn):
        swap(i).wait_recv()
        zz = lax.rem(z + outs[i], zn)
        both = p[pl.ds(pl.multiple_of((2 * zz + c) * T, 16), T), :].astype(F32) + xr[i].astype(F32)
        if i < zn - 1:
            cb[i] = both.astype(BF16)
            reduce_to(i).start()
        else:
            own = both
    for i in range(zn - 1):
        reduce_to(i).wait_recv()
        own = own + zr[i].astype(F32)
    st = (tok[...].astype(F32) + own).astype(BF16)
    out[...] = st
    wide = st.astype(F32)
    inverse = lax.rsqrt(jnp.mean(wide * wide, axis=1, keepdims=True) + 1e-05)
    ng[0] = (wide * inverse * gain[...]).astype(BF16)
    for i in range(1, zn):
        spread(i).start()
    dispatch(0)
    if zn > 1:
        dispatch(1)
    for load in loads:
        load.wait()
    for i in range(zn):
        pass_on(i)
        if i + 2 < zn:
            dispatch(i + 2)
        expert(i)
        if i >= 1:
            give_back(i - 1)
        if i >= 2:
            mix(i - 2)
    give_back(zn - 1)
    if zn > 1:
        mix(zn - 2)
    mix(zn - 1)
    total = out[...].astype(F32) + keep[...]
    for i in range(1, zn):
        reduce_out(i).wait_recv()
        total = total + rr[i].astype(F32)
    out[...] = total.astype(BF16)
    for i in range(zn):
        swap(i).wait_send()
        if i < zn - 1:
            reduce_to(i).wait_send()
        if i > 0:
            spread(i).wait_send()
            reduce_out(i).wait_send()
            for n in range(2):
                aux(n, i).wait_send()

        def drain(d, _):
            forward(i, d).wait_send()
            swap_out(i, d).wait_send()
            return 0

        lax.fori_loop(0, sp, drain, 0)
        for d in range(1, sp):
            route(i, d).wait_send()
            back(i, d, s).wait_send()


def params(cid=None):
    if cid is None:
        return pltpu.CompilerParams(vmem_limit_bytes=VMEM_LIMIT)
    return pltpu.CompilerParams(
        collective_id=cid, has_side_effects=True, vmem_limit_bytes=VMEM_LIMIT
    )


def shards(
    tokens,
    query_vectors,
    key_vectors,
    value_vectors,
    cum_gate,
    out_weight,
    norm_gain,
    gate_weight,
    up_weight,
    down_weight,
    expert_ids,
    route_weights,
):
    sp = lax.axis_size("sp")
    tp = lax.axis_size("tp")
    zn = tp // 2
    seg, width = query_vectors.shape
    heads = cum_gate.shape[1]
    T, D = tokens.shape
    dma = pltpu.SemaphoreType.DMA

    n_experts = gate_weight.shape[0] * sp
    top = expert_ids.shape[1]
    cap = max(2, 3 * T * top // (2 * n_experts))
    cap = -(-cap // 8) * 8
    slots = n_experts * cap
    flat = expert_ids.reshape(-1)
    hits = (flat[:, None] == jnp.arange(n_experts, dtype=jnp.int32)[None, :]).astype(F32)
    lower = jnp.tril(jnp.ones((flat.shape[0], flat.shape[0]), F32), -1)
    earlier = jnp.dot(lower, hits, preferred_element_type=F32)
    slot = (flat * cap + jnp.sum(earlier * hits, axis=1).astype(jnp.int32)).reshape(T, top)
    match = slot[:, :, None] == jnp.arange(slots, dtype=jnp.int32)[None, None, :]
    place = jnp.any(match, axis=1).astype(BF16).T
    weight = jnp.sum(jnp.where(match, route_weights[:, :, None], 0.0), axis=1)
    high = lax.reduce_precision(weight, 8, 7)
    comb = jnp.concatenate([high, weight - high], axis=0).astype(BF16)

    fh = gate_weight.shape[2]
    partial = pl.pallas_call(
        functools.partial(attend_kernel, sp, heads),
        out_shape=jax.ShapeDtypeStruct((seg, D), BF16),
        in_specs=vmem_specs(5),
        out_specs=vmem_specs(1)[0],
        scratch_shapes=[
            pltpu.VMEM((sp, seg, width), BF16),
            pltpu.VMEM((sp, seg, width), BF16),
            pltpu.VMEM((sp, heads, seg), F32),
            pltpu.VMEM((seg, width), BF16),
            pltpu.VMEM((heads, seg, 1), F32),
            pltpu.VMEM((heads, seg, 1), F32),
            pltpu.VMEM((heads, seg, width // heads), F32),
            dma((3, sp)), dma((3, sp)),
        ],
        compiler_params=params(0),
        name="attend",
    )(query_vectors, key_vectors, value_vectors, cum_gate.T, out_weight)

    def vm(*shape, kind=BF16):
        return pltpu.VMEM(shape, kind)

    return pl.pallas_call(
        functools.partial(experts_kernel, sp, zn),
        out_shape=jax.ShapeDtypeStruct((T, D), BF16),
        in_specs=vmem_specs(5) + [pl.BlockSpec(memory_space=pl.ANY)] * 3,
        out_specs=vmem_specs(1)[0],
        scratch_shapes=[
            vm(D, fh), vm(D, fh), vm(fh, D),
            vm(zn, T, D), vm(zn, T, D), vm(zn, T, D), vm(zn, T, D),
            vm(zn, slots, T), vm(zn, 2 * T, slots),
            vm(zn, sp, cap, D),
            vm(zn, sp, 2, cap, D),
            vm(sp * 2 * cap, fh),
            vm(zn, sp, 2, cap, D),
            vm(zn, sp, cap, D), vm(zn, sp, cap, D), vm(zn, sp, cap, D),
            vm(zn, T, D), vm(zn, T, D),
            vm(T, D, kind=F32),
            dma((3,)),
            dma((zn,)), dma((zn,)),
            dma((2, zn)), dma((2, zn)),
            dma((zn,)), dma((zn,)),
            dma((zn,)), dma((zn,)),
            dma((zn, sp)), dma((zn, sp)),
            dma((zn, sp)), dma((zn, sp)),
            dma((zn, sp)), dma((zn, sp)),
            dma((zn, sp)), dma((zn, sp)),
            dma((zn,)), dma((zn,)),
        ],
        compiler_params=params(1),
        name="experts",
    )(partial, tokens, norm_gain[None, :], place, comb, gate_weight, up_weight, down_weight)


def solution(mesh):
    in_specs = (
        P(("sp", "tp"), None),
        P("sp", "tp"),
        P("sp", "tp"),
        P("sp", "tp"),
        P("sp", "tp"),
        P("tp", None),
        P(),
        P("sp", None, "tp"),
        P("sp", None, "tp"),
        P("sp", "tp", None),
        P(("sp", "tp"), None),
        P(("sp", "tp"), None),
    )
    out_specs = P(("sp", "tp"), None)
    return jax.shard_map(shards, mesh=mesh, in_specs=in_specs, out_specs=out_specs, check_vma=False)
```
